32 devices in a mesh: fs: 8 (over z, x), tp: 4 (over y, core).
Axes of the slice: x: 2, y: 2, z: 4, core: 2. Of those that a mesh axis runs over, the one named last changes fastest.
Arguments:
- normed_input: bfloat16 [16384, 2048], P('fs'), may hold values from -6 to 6
- gate_cotangent: bfloat16 [16384, 2048], P('fs', 'tp'), may hold values from -0.125 to 0.125
- first_value_cot: bfloat16 [16384, 1024], P('fs', 'tp'), may hold values from -0.125 to 0.125
- second_value_cot: bfloat16 [16384, 1024], P('fs', 'tp'), may hold values from -0.125 to 0.125
- head_lambda: float32 [8], P('tp'), may hold values from 0.3 to 0.8
- projection: bfloat16 [2048, 256], replicated, may hold values from -1 to 1, as said below
- gate_weight: float32 [2048, 2048], P('fs', 'tp'), may hold values from -0.125 to 0.125
- gate_first: float32 [256, 2048], P('fs', 'tp'), may hold values from -1.5 to 1.5
- gate_second: float32 [256, 2048], P('fs', 'tp'), may hold values from 0.01 to 1
- value_weight: float32 [2048, 1024], P('fs', 'tp'), may hold values from -0.125 to 0.125
- value_first: float32 [256, 1024], P('fs', 'tp'), may hold values from -1.5 to 1.5
- value_second: float32 [256, 1024], P('fs', 'tp'), may hold values from 0.01 to 1
Outputs:
- new_gate_weight: float32 [2048, 2048], P('fs', 'tp')
- gate_step: float32 [2048, 2048], P('fs', 'tp')
- gate_copy: bfloat16 [2048, 2048], P(None, 'tp')
- new_gate_first: float32 [256, 2048], P('fs', 'tp')
- new_gate_second: float32 [256, 2048], P('fs', 'tp')
- new_value_weight: float32 [2048, 1024], P('fs', 'tp')
- value_step: float32 [2048, 1024], P('fs', 'tp')
- value_copy: bfloat16 [2048, 1024], P(None, 'tp')
- new_value_first: float32 [256, 1024], P('fs', 'tp')
- new_value_second: float32 [256, 1024], P('fs', 'tp')
The draws below stay inside these ranges and needn't reach their ends.
Inputs may be any that keep to these rules, and one draw needn't show every extreme that they name: `projection`: a low-rank factor whose rows differ in scale.
All inputs are finite; a program needn't handle non-finite values.
Results may differ from the reference program's by a relative error of at most 0.0054.
Values may be sent and summed in bfloat16 or wider, within the bound.
No kernel may reach another device: no remote copies, remote signals or barrier semaphores. Data moves between devices by JAX's collectives and lax.ppermute only.
A program may use at most 64 MiB of HBM per device.

```python
import math
import jax
import jax.numpy as jnp
from jax import lax

D = 2048
HEADS = 8
VDIM = 128
RANK = 256
TOKENS = 16384


def draw_projection(key, part):
    noise_key = jax.random.fold_in(key, 11)
    rough_key = jax.random.fold_in(key, 12)
    phase_key = jax.random.fold_in(key, 13)
    row_place = jnp.arange(D, dtype=jnp.float32)[:, None] / D
    phase = jax.random.uniform(phase_key, (), jnp.float32, 0.0, 6.2832)
    slow = jnp.exp(1.2 * jnp.sin(12.566 * row_place + phase))
    rough = jnp.exp(jax.random.uniform(rough_key, (D, 1), jnp.float32, -0.5, 0.5))
    base = jax.random.normal(noise_key, (D, RANK), jnp.float32)
    value = base * slow * rough * D ** (-0.5)
    return jnp.clip(value, -1.0, 1.0).astype(jnp.bfloat16)


def raised(entries, key, source, target, shards_of, factor):
    owner, partner = [(jnp.arange(entries.shape[axis_at]) // (entries.shape[axis_at] // shards_of)).reshape([-1 if axis == axis_at else 1 for axis in range(entries.ndim)]) for axis_at in (source, target)]
    chosen = jax.random.permutation(key, shards_of)[partner]
    strong = (owner == chosen) | (owner == (partner + shards_of // 2) % shards_of)
    return jnp.where(strong, factor * entries, entries)


def steps_of(key, dims, split, smallest, largest):
    loudness = 1.0
    for axis_at, blocks in split:
        heights = jax.random.uniform(jax.random.fold_in(jax.random.fold_in(key, 6), axis_at), (blocks,), jnp.float32, smallest / len(split), largest / len(split))
        loudness = loudness * jnp.repeat(jnp.exp(heights), dims[axis_at] // blocks).reshape((-1,) + (1,) * (len(dims) - 1 - axis_at))
    return loudness


def noise(own_key, dims, spread, bound, cuts=(), held_as=jnp.bfloat16):
    array = spread * jax.random.normal(own_key, dims, jnp.float32)
    if cuts:
        array = array * steps_of(own_key, dims, cuts, -0.22, 0.18)
    return jnp.clip(array, -bound, bound).astype(held_as)


def gaussian_with(key, extent, deviation, limit, shards, heavy, kind=jnp.bfloat16):
    array = deviation * jax.random.normal(key, extent, jnp.float32)
    if shards:
        array = array * steps_of(key, extent, shards, -0.22, 0.18)
    return jnp.clip(raised(array, jax.random.fold_in(key, 3), *heavy), -limit, limit).astype(kind)


def setup_inputs(seed: int = 0) -> dict:
    splits = jax.random.split(jax.random.key(seed), 13)
    return {
        "normed_input": gaussian_with(splits[0], (TOKENS, D), 1.0, 6.0, ((0, 8),), (0, 1, 8, 2.0)),
        "gate_cotangent": noise(splits[1], (TOKENS, D), (TOKENS ** -0.5), 0.125, ((0, 8), (1, 4))),
        "first_value_cot": noise(splits[2], (TOKENS, HEADS * VDIM), (TOKENS ** -0.5), 0.125, ((0, 8), (1, 4))),
        "second_value_cot": noise(splits[3], (TOKENS, HEADS * VDIM), (TOKENS ** -0.5), 0.125, ((0, 8), (1, 4))),
        "head_lambda": jnp.clip(0.3 + 0.5 * jax.random.uniform(splits[4], (HEADS,), jnp.float32) ** steps_of(splits[4], (HEADS,), ((0, 4),), -0.2, 0.2), 0.3, 0.8),
        "projection": draw_projection(jax.random.fold_in(splits[12], 71), 0),
        "gate_weight": noise(splits[6], (D, D), D ** -0.5, 0.125, ((0, 8), (1, 4)), jnp.float32),
        "gate_first": noise(splits[7], (RANK, D), 0.1, 1.5, ((0, 8), (1, 4)), jnp.float32),
        "gate_second": jnp.clip(jnp.exp(math.log(1.0) - 4.6051702 * jax.random.uniform(splits[8], (RANK, D), jnp.float32) ** steps_of(splits[8], (RANK, D), ((0, 8), (1, 4)), -0.2, 0.2)), 0.01, 1.0),
        "value_weight": noise(splits[9], (D, HEADS * VDIM), D ** -0.5, 0.125, ((0, 8), (1, 4)), jnp.float32),
        "value_first": noise(splits[10], (RANK, HEADS * VDIM), 0.1, 1.5, ((0, 8), (1, 4)), jnp.float32),
        "value_second": jnp.clip(jnp.exp(math.log(1.0) - 4.6051702 * jax.random.uniform(splits[11], (RANK, HEADS * VDIM), jnp.float32) ** steps_of(splits[11], (RANK, HEADS * VDIM), ((0, 8), (1, 4)), -0.2, 0.2)), 0.01, 1.0),
    }


moment_decay = 0.9
square_decay = 0.95
adam_floor = 1e-08
learn_rate = 0.02
rms_floor = 0.1

def across_tokens(left, right):
    return lax.dot_general(left, right, (((0,), (0,)), ((), ())), preferred_element_type=jnp.float32)

def optimizer_step(weight, first, second, gradient, projection):
    factor = projection.astype(jnp.float32)
    low = lax.dot_general(factor, gradient, (((0,), (0,)), ((), ())), precision=lax.Precision.HIGHEST)
    new_first = moment_decay * first + (1.0 - moment_decay) * low
    new_second = square_decay * second + (1.0 - square_decay) * low * low
    direction = new_first / (jnp.sqrt(new_second) + adam_floor)
    update = jnp.dot(factor, direction, precision=lax.Precision.HIGHEST)
    step = update / (jnp.sqrt(jnp.mean(update * update)) + rms_floor)
    new_weight = weight - learn_rate * step
    return (new_weight, step, new_weight.astype(jnp.bfloat16), new_first, new_second)

def reference(normed_input, gate_cotangent, first_value_cot, second_value_cot, head_lambda, projection, gate_weight, gate_first, gate_second, value_weight, value_first, value_second):
    column_lambda = jnp.repeat(head_lambda, VDIM)
    value_cot = (first_value_cot.astype(jnp.float32) - column_lambda[None, :] * second_value_cot.astype(jnp.float32)).astype(jnp.bfloat16)
    gate_grad = across_tokens(normed_input, gate_cotangent)
    value_grad = across_tokens(normed_input, value_cot)
    gate_parts = optimizer_step(gate_weight, gate_first, gate_second, gate_grad, projection)
    value_parts = optimizer_step(value_weight, value_first, value_second, value_grad, projection)
    return (gate_parts[0], gate_parts[1], gate_parts[2], gate_parts[3], gate_parts[4], value_parts[0], value_parts[1], value_parts[2], value_parts[3], value_parts[4])
```

```python
import jax
import jax.numpy as jnp
from jax import lax
from jax.experimental import pallas as pl
from jax.experimental.pallas import tpu as pltpu
from jax.sharding import PartitionSpec as P

moment_decay = 0.9
square_decay = 0.95
adam_floor = 1e-08
learn_rate = 0.02
rms_floor = 0.1


f32 = jnp.float32
bf16 = jnp.bfloat16


def params(vmem_mib=48, **kw):
    return pltpu.CompilerParams(vmem_limit_bytes=vmem_mib << 20, **kw)


def shape(dims, dtype):
    return jax.ShapeDtypeStruct(dims, dtype)


def inner_of(fs):
    inner = 1
    while inner * inner * 2 < fs:
        inner *= 2
    return inner


def exchange(value, axis, size, bit):
    return lax.ppermute(value, axis, [(i, i ^ bit) for i in range(size)])


def partial_kernel(place, lam, x, p, gate, first, second, *rest):
    outs, total = rest[:-1], rest[-1]
    step = pl.program_id(0)
    heads = lam.shape[0]
    wide = first.shape[1] // heads
    low = jnp.dot(x[...], p[...], preferred_element_type=f32).astype(bf16)
    cot = [gate[...]]
    for h in range(heads):
        cols = slice(h * wide, (h + 1) * wide)
        cot.append((first[:, cols].astype(f32) - lam[h] * second[:, cols].astype(f32)).astype(bf16))
    part = lax.dot_general(
        low, jnp.concatenate(cot, 1), (((0,), (0,)), ((), ())), preferred_element_type=f32
    )

    @pl.when(step == 0)
    def _():
        total[...] = part

    @pl.when(step > 0)
    def _():
        total[...] += part

    @pl.when(step == pl.num_programs(0) - 1)
    def _():
        rows = total.shape[0] // len(outs)
        for k, out in enumerate(outs):
            at = pl.multiple_of(lax.bitwise_xor(place[0], jnp.int32(k)) * rows, rows)
            out[...] = total[pl.ds(at, rows), :].astype(out.dtype)


def partial_call(place, x, gate, first, second, lam, p, outer, blocks=2):
    tokens, depth = x.shape
    factors = p.shape[1]
    block = tokens // blocks
    width = gate.shape[1] + first.shape[1]
    rows = factors // outer
    return pl.pallas_call(
        partial_kernel,
        grid_spec=pltpu.PrefetchScalarGridSpec(
            num_scalar_prefetch=2,
            grid=(blocks,),
            in_specs=[
                pl.BlockSpec((block, depth), lambda i, *_: (i, 0)),
                pl.BlockSpec((depth, factors), lambda i, *_: (0, 0)),
                pl.BlockSpec((block, gate.shape[1]), lambda i, *_: (i, 0)),
                pl.BlockSpec((block, first.shape[1]), lambda i, *_: (i, 0)),
                pl.BlockSpec((block, first.shape[1]), lambda i, *_: (i, 0)),
            ],
            out_specs=[pl.BlockSpec((rows, width), lambda i, *_: (0, 0))] * outer,
            scratch_shapes=[pltpu.VMEM((factors, width), f32)],
        ),
        out_shape=[shape((rows, width), f32 if k == 0 else bf16) for k in range(outer)],
        compiler_params=params(dimension_semantics=("arbitrary",)),
        name="partial",
    )(place, lam, x, p, gate, first, second)


def sum_kernel(*refs):
    total = refs[0][...]
    for ref in refs[1:-1]:
        total = total + ref[...].astype(f32)
    refs[-1][...] = total.astype(bf16)


def sum_call(parts):
    return pl.pallas_call(
        sum_kernel, out_shape=shape(parts[0].shape, bf16), compiler_params=params(), name="slab_sum"
    )(*parts)


def moment_kernel(inner, place, *refs):
    sums, held = refs[:inner], refs[inner : 2 * inner]
    gate_first, gate_second, value_first, value_second = refs[2 * inner : 2 * inner + 4]
    direction, ngf, ngs, nvf, nvs = refs[2 * inner + 4 : 2 * inner + 9]
    order, low = refs[2 * inner + 9 :]
    own = place[0]
    rows = gate_first.shape[0]
    split = gate_first.shape[1]
    for k in range(inner):
        order[lax.bitwise_xor(own, jnp.int32(k))] = sums[k][...].astype(f32)
    total = order[0]
    for k in range(1, inner):
        total = total + order[k]
    low[...] = total
    for k in range(inner):
        at = pl.multiple_of(lax.bitwise_xor(own, jnp.int32(k)) * rows, rows)
        grad = low[pl.ds(at, rows), :]
        first = moment_decay * held[k][:rows, :].astype(f32) + (1.0 - moment_decay) * grad
        second = square_decay * held[k][rows:, :].astype(f32) + (1.0 - square_decay) * grad * grad
        direction[pl.ds(at, rows), :] = (first / (jnp.sqrt(second) + adam_floor)).astype(bf16)
    grad = low[pl.ds(pl.multiple_of(own * rows, rows), rows), :]
    g, v = grad[:, :split], grad[:, split:]
    ngf[...] = moment_decay * gate_first[...] + (1.0 - moment_decay) * g
    nvf[...] = moment_decay * value_first[...] + (1.0 - moment_decay) * v
    ngs[...] = square_decay * gate_second[...] + (1.0 - square_decay) * g * g
    nvs[...] = square_decay * value_second[...] + (1.0 - square_decay) * v * v


def moment_call(place, sums, held, gate_first, gate_second, value_first, value_second):
    inner = len(sums)
    slab = sums[0].shape
    vmem = pl.BlockSpec(memory_space=pltpu.VMEM)
    return pl.pallas_call(
        lambda *refs: moment_kernel(inner, *refs),
        in_specs=[pl.BlockSpec(memory_space=pltpu.SMEM)] + [vmem] * (2 * inner + 4),
        out_specs=[vmem] * 5,
        out_shape=[
            shape(slab, bf16),
            shape(gate_first.shape, f32),
            shape(gate_first.shape, f32),
            shape(value_first.shape, f32),
            shape(value_first.shape, f32),
        ],
        scratch_shapes=[pltpu.VMEM((inner,) + slab, f32), pltpu.VMEM(slab, f32)],
        compiler_params=params(),
        name="moments",
    )(place, *sums, *held, gate_first, gate_second, value_first, value_second)


def gram_kernel(p, upper, lower):
    gram = lax.dot_general(p[...], p[...], (((0,), (0,)), ((), ())), preferred_element_type=f32)
    high = gram.astype(bf16)
    upper[...] = high
    lower[...] = (gram - high.astype(f32)).astype(bf16)


def gram_call(p):
    dims = (p.shape[1], p.shape[1])
    return pl.pallas_call(
        gram_kernel, out_shape=[shape(dims, bf16)] * 2, compiler_params=params(), name="gram"
    )(p)


def square_kernel(outer, split, place, *refs):
    slabs, (upper, lower, full, squares) = refs[:outer], refs[outer:]
    rows = slabs[0].shape[0]
    for k in range(outer):
        at = pl.multiple_of(lax.bitwise_xor(place[0], jnp.int32(k)) * rows, rows)
        full[pl.ds(at, rows), :] = slabs[k][...]
    d = full[...]
    image = jnp.dot(upper[...], d, preferred_element_type=f32)
    image += jnp.dot(lower[...], d, preferred_element_type=f32)
    products = jnp.sum(image * d.astype(f32), axis=0, keepdims=True)
    gate = jnp.sum(products[:, :split], axis=1, keepdims=True)
    value = jnp.sum(products[:, split:], axis=1, keepdims=True)
    row = lax.broadcasted_iota(jnp.int32, squares.shape, 0)
    squares[...] = jnp.where(row == 0, gate, value)


def square_call(place, slabs, upper, lower, split):
    outer = len(slabs)
    rows, width = slabs[0].shape
    vmem = pl.BlockSpec(memory_space=pltpu.VMEM)
    return pl.pallas_call(
        lambda *refs: square_kernel(outer, split, *refs),
        in_specs=[pl.BlockSpec(memory_space=pltpu.SMEM)] + [vmem] * (outer + 2),
        out_specs=[vmem] * 2,
        out_shape=[shape((rows * outer, width), bf16), shape((8, 128), f32)],
        compiler_params=params(),
        name="squares",
    )(place, *slabs, upper, lower)


def final_kernel(count, entries, place, *refs):
    weights = refs[:count]
    mine, theirs, d, p, gate_weight, value_weight = refs[count : count + 6]
    new_gate, gate_step, gate_copy, new_value, value_step, value_copy = refs[count + 6 :]
    step = pl.program_id(0)
    split = gate_weight.shape[1]
    both = mine[...] + theirs[...]
    scale = [1.0 / (jnp.sqrt(both[i : i + 1, :1] / entries[i]) + rms_floor) for i in range(2)]
    update = jnp.dot(p[...], d[...], preferred_element_type=f32)
    gate, value = update[:, :split] * scale[0], update[:, split:] * scale[1]
    for k in range(count):

        @pl.when(step == k)
        def _():
            old = weights[k][...].astype(f32)
            gate_copy[...] = (old[:, :split] - learn_rate * gate).astype(bf16)
            value_copy[...] = (old[:, split:] - learn_rate * value).astype(bf16)

    @pl.when(step == 0)
    def _():
        gate_step[...] = gate
        value_step[...] = value
        new_gate[...] = gate_weight[...] - learn_rate * gate
        new_value[...] = value_weight[...] - learn_rate * value


def final_call(place, weights, mine, theirs, d, p, gate_weight, value_weight, columns):
    count = len(weights)
    rows, split = gate_weight.shape
    rest = value_weight.shape[1]
    width = split + rest
    factors = p.shape[1]
    whole = lambda dims: pl.BlockSpec(dims, lambda i, place: (0, 0))
    moved = lambda dims: pl.BlockSpec(dims, lambda i, place: (lax.bitwise_xor(place[0], i), 0))
    entries = (rows * count * split * columns, rows * count * rest * columns)
    return pl.pallas_call(
        lambda *refs: final_kernel(count, entries, *refs),
        grid_spec=pltpu.PrefetchScalarGridSpec(
            num_scalar_prefetch=1,
            grid=(count,),
            in_specs=[whole((rows, width))] * count
            + [
                whole((8, 128)),
                whole((8, 128)),
                whole((factors, width)),
                moved((rows, factors)),
                whole((rows, split)),
                whole((rows, rest)),
            ],
            out_specs=[
                whole((rows, split)),
                whole((rows, split)),
                moved((rows, split)),
                whole((rows, rest)),
                whole((rows, rest)),
                moved((rows, rest)),
            ],
        ),
        out_shape=[
            shape((rows, split), f32),
            shape((rows, split), f32),
            shape((rows * count, split), bf16),
            shape((rows, rest), f32),
            shape((rows, rest), f32),
            shape((rows * count, rest), bf16),
        ],
        compiler_params=params(dimension_semantics=("arbitrary",)),
        name="final",
    )(place, *weights, mine, theirs, d, p, gate_weight, value_weight)


def solution(mesh):
    fs, tp = mesh.shape["fs"], mesh.shape["tp"]
    inner = inner_of(fs)
    outer = fs // inner

    def per_device(
        normed_input,
        gate_cotangent,
        first_value_cot,
        second_value_cot,
        head_lambda,
        projection,
        gate_weight,
        gate_first,
        gate_second,
        value_weight,
        value_first,
        value_second,
    ):
        index = lax.axis_index("fs").astype(jnp.int32)
        here = index.reshape(1)
        z = (index // inner).reshape(1)
        x = (index % inner).reshape(1)
        held = jnp.concatenate(
            [
                jnp.concatenate([gate_first, value_first], 1),
                jnp.concatenate([gate_second, value_second], 1),
            ],
            0,
        ).astype(bf16)
        weight = jnp.concatenate([gate_weight, value_weight], 1).astype(bf16)
        weights = [weight] + [exchange(weight, "fs", fs, k) for k in range(1, fs)]
        held_by = [held] + [exchange(held, "fs", fs, k) for k in range(1, inner)]
        upper, lower = gram_call(projection)
        parts = partial_call(
            z, normed_input, gate_cotangent, first_value_cot, second_value_cot, head_lambda, projection, outer
        )
        summed = sum_call([parts[0]] + [exchange(parts[k], "fs", fs, k * inner) for k in range(1, outer)])
        sums = [summed] + [exchange(summed, "fs", fs, k) for k in range(1, inner)]
        direction, ngf, ngs, nvf, nvs = moment_call(
            x, sums, held_by, gate_first, gate_second, value_first, value_second
        )
        slabs = [direction] + [exchange(direction, "fs", fs, k * inner) for k in range(1, outer)]
        full, squares = square_call(z, slabs, upper, lower, gate_cotangent.shape[1])
        bit = 1
        while bit * 2 < tp:
            squares = squares + exchange(squares, "tp", tp, bit)
            bit *= 2
        new_gate, gate_step, gate_copy, new_value, value_step, value_copy = final_call(
            here, weights, squares, exchange(squares, "tp", tp, bit), full, projection, gate_weight, value_weight, tp
        )
        return (
            new_gate,
            gate_step,
            gate_copy,
            ngf,
            ngs,
            new_value,
            value_step,
            value_copy,
            nvf,
            nvs,
        )

    blocked = P("fs", "tp")
    return jax.shard_map(
        per_device,
        mesh=mesh,
        in_specs=(P("fs", None), blocked, blocked, blocked, P("tp"), P()) + (blocked,) * 6,
        out_specs=(blocked, blocked, P(None, "tp"), blocked, blocked, blocked, blocked, P(None, "tp"), blocked, blocked),
        check_vma=False,
    )
```

```python
import jax
import jax.numpy as jnp
from jax import lax
from jax.experimental import pallas as pl
from jax.experimental.pallas import tpu as pltpu
from jax.sharding import PartitionSpec as P


moment_decay = 0.9
square_decay = 0.95
adam_floor = 1e-08
learn_rate = 0.02
rms_floor = 0.1


f32 = jnp.float32
bf16 = jnp.bfloat16
partial_vmem_mib = 54


def params(vmem_mib=4, **kw):
    return pltpu.CompilerParams(vmem_limit_bytes=int(vmem_mib * 2**20), **kw)


def shape(dims, dtype):
    return jax.ShapeDtypeStruct(dims, dtype)


def inner_of(fs):
    inner = 1
    while inner * inner * 2 < fs:
        inner *= 2
    return inner


def exchange(value, axis, size, bit):
    return lax.ppermute(value, axis, [(i, i ^ bit) for i in range(size)])


VMEM = pl.BlockSpec(memory_space=pltpu.VMEM)
SMEM = pl.BlockSpec(memory_space=pltpu.SMEM)
HBM = pl.BlockSpec(memory_space=pltpu.MemorySpace.HBM)


def cast_kernel(gate, value, out, gate_here, value_here, sems):
    split = gate.shape[1]
    copies = [
        pltpu.make_async_copy(gate, gate_here, sems.at[0]),
        pltpu.make_async_copy(value, value_here, sems.at[1]),
    ]
    for copy in copies:
        copy.start()
    copies[0].wait()
    out[:, :split] = gate_here[...].astype(bf16)
    copies[1].wait()
    out[:, split:] = value_here[...].astype(bf16)


def cast_call(gate, value):
    dims = (gate.shape[0], gate.shape[1] + value.shape[1])
    return pl.pallas_call(
        cast_kernel,
        in_specs=[HBM] * 2,
        out_specs=VMEM,
        out_shape=shape(dims, bf16),
        scratch_shapes=[
            pltpu.VMEM(gate.shape, f32),
            pltpu.VMEM(value.shape, f32),
            pltpu.SemaphoreType.DMA((2,)),
        ],
        compiler_params=params(62),
        name="cast",
    )(gate, value)


def partial_kernel(inner, cuts, place, lam, x, p, gate, first, second, *rest):
    outs = rest[:inner]
    x_here, p_here, gate_here, first_here, second_here, low, total, block_sems, sems = rest[inner:]
    count, ahead = len(cuts), 2
    heads = lam.shape[0]
    split = gate.shape[1]
    wide = first.shape[1] // heads
    unit = x.shape[0] // sum(cuts)
    at = [pl.ds(sum(cuts[:i]) * unit, cuts[i] * unit) for i in range(count)]
    blocks = [pltpu.make_async_copy(x.at[r], x_here.at[r], block_sems.at[i]) for i, r in enumerate(at)]
    pairs = (p, p_here), (gate, gate_here), (first, first_here), (second, second_here)
    p_load, gate_load, *value_loads = [pltpu.make_async_copy(a, b, sems.at[i]) for i, (a, b) in enumerate(pairs)]
    p_load.start()
    for i in range(ahead):
        blocks[i].start()
    p_load.wait()
    for i in range(count):
        blocks[i].wait()
        if i + ahead < count:
            blocks[i + ahead].start()
        if i + ahead == count - 1:
            for load in value_loads:
                load.start()
            gate_load.start()
        if i == count - 1:
            for load in value_loads:
                load.wait()
            cot = []
            for h in range(heads):
                cols = slice(h * wide, (h + 1) * wide)
                cot.append((first_here[:, cols].astype(f32) - lam[h] * second_here[:, cols].astype(f32)).astype(bf16))
            value = jnp.concatenate(cot, 1)
        low[at[i], :] = jnp.dot(x_here[at[i], :], p_here[...], preferred_element_type=f32).astype(bf16)
    over_tokens = (((0,), (0,)), ((), ()))
    total[:, split:] = lax.dot_general(low[...], value, over_tokens, preferred_element_type=f32)
    gate_load.wait()
    total[:, :split] = lax.dot_general(low[...], gate_here[...], over_tokens, preferred_element_type=f32)
    outer, height = outs[0].shape[:2]
    for k, out in enumerate(outs):
        for j in range(outer):
            here = lax.bitwise_xor(place[0], jnp.int32(j * inner + k)) * height
            out[j] = total[pl.ds(pl.multiple_of(here, height), height), :].astype(out.dtype)


def partial_call(place, x, gate, first, second, lam, p, outer, inner, cuts=(1, 2, 3, 2)):
    factors = p.shape[1]
    width = gate.shape[1] + first.shape[1]
    dims = (outer, factors // (outer * inner), width)
    return pl.pallas_call(
        lambda *refs: partial_kernel(inner, cuts, *refs),
        in_specs=[SMEM] * 2 + [HBM] * 5,
        out_specs=[VMEM] * inner,
        out_shape=[shape(dims, f32 if k == 0 else bf16) for k in range(inner)],
        scratch_shapes=[pltpu.VMEM(a.shape, bf16) for a in (x, p, gate, first, second)]
        + [
            pltpu.VMEM((x.shape[0], factors), bf16),
            pltpu.VMEM((factors, width), f32),
            pltpu.SemaphoreType.DMA((len(cuts),)),
            pltpu.SemaphoreType.DMA((4,)),
        ],
        compiler_params=params(partial_vmem_mib),
        name="partial",
    )(place, lam, x, p, gate, first, second)


def sum_kernel(count, *refs):
    parts, outs = refs[:count], refs[count:]
    for j, out in enumerate(outs):
        total = parts[0][j]
        for part in parts[1:]:
            total = total + part[j].astype(f32)
        out[...] = total.astype(out.dtype)


def sum_call(parts):
    outer, rows, width = parts[0].shape
    return pl.pallas_call(
        lambda *refs: sum_kernel(len(parts), *refs),
        out_shape=[shape((rows, width), f32 if j == 0 else bf16) for j in range(outer)],
        compiler_params=params(),
        name="slab_sum",
    )(*parts)


def advanced(low, gate_first, gate_second, value_first, value_second):
    split = gate_first.shape[1]
    for first, second, cols in (
        (gate_first, gate_second, slice(None, split)),
        (value_first, value_second, slice(split, None)),
    ):
        grad = low[:, cols]
        moved = moment_decay * first[...] + (1.0 - moment_decay) * grad
        yield cols, moved, square_decay * second[...] + (1.0 - square_decay) * grad * grad


def direct_kernel(count, *refs):
    parts = refs[:count]
    gate_first, gate_second, value_first, value_second, direction, low_out = refs[count:]
    low = parts[0][...]
    for part in parts[1:]:
        low = low + part[...].astype(f32)
    low_out[...] = low
    for cols, moved, squared in advanced(low, gate_first, gate_second, value_first, value_second):
        direction[:, cols] = (moved / (jnp.sqrt(squared) + adam_floor)).astype(bf16)


def direct_call(parts, moments):
    return pl.pallas_call(
        lambda *refs: direct_kernel(len(parts), *refs),
        out_shape=[shape(parts[0].shape, bf16), shape(parts[0].shape, f32)],
        compiler_params=params(),
        name="direct",
    )(*parts, *moments)


def store_kernel(low, gate_first, gate_second, value_first, value_second, *outs):
    new = advanced(low[...], gate_first, gate_second, value_first, value_second)
    for i, (_, moved, squared) in enumerate(new):
        outs[2 * i][...] = moved
        outs[2 * i + 1][...] = squared


def store_call(low, moments):
    return pl.pallas_call(
        store_kernel,
        out_shape=[shape(moment.shape, f32) for moment in moments],
        compiler_params=params(),
        name="store",
    )(low, *moments)


def gram_kernel(p, half, upper, lower, half_here):
    half_here[...] = half[...]
    gram = lax.dot_general(p[...], p[...], (((0,), (0,)), ((), ())), preferred_element_type=f32)
    high = gram.astype(bf16)
    upper[...] = high
    lower[...] = (gram - high.astype(f32)).astype(bf16)


def gram_call(p, half):
    dims = (p.shape[1], p.shape[1])
    return pl.pallas_call(
        gram_kernel,
        out_shape=[shape(dims, bf16)] * 2 + [shape(half.shape, half.dtype)],
        compiler_params=params(),
        name="gram",
    )(p, half)


def square_kernel(count, split, place, *refs):
    slabs, (upper, lower, full, squares, wide) = refs[:count], refs[count:]
    rows = slabs[0].shape[0]
    for k in range(count):
        at = pl.multiple_of(lax.bitwise_xor(place[0], jnp.int32(k)) * rows, rows)
        wide[pl.ds(at, rows), :] = slabs[k][...].astype(f32)
    d = wide[...].astype(bf16)
    full[...] = d
    image = jnp.dot(upper[...], d, preferred_element_type=f32)
    image += jnp.dot(lower[...], d, preferred_element_type=f32)
    products = jnp.sum(image * d.astype(f32), axis=0, keepdims=True)
    gate = jnp.sum(products[:, :split], axis=1, keepdims=True)
    value = jnp.sum(products[:, split:], axis=1, keepdims=True)
    row = lax.broadcasted_iota(jnp.int32, squares.shape, 0)
    squares[...] = jnp.where(row == 0, gate, value)


def square_call(place, slabs, upper, lower, split):
    count = len(slabs)
    rows, width = slabs[0].shape
    return pl.pallas_call(
        lambda *refs: square_kernel(count, split, *refs),
        in_specs=[SMEM] + [VMEM] * (count + 2),
        out_specs=[VMEM] * 2,
        out_shape=[shape((rows * count, width), bf16), shape((8, 128), f32)],
        scratch_shapes=[pltpu.VMEM((rows * count, width), f32)],
        compiler_params=params(8),
        name="squares",
    )(place, *slabs, upper, lower)


def update_kernel(p, d, out):
    out[...] = jnp.dot(p[...], d[...], preferred_element_type=f32)


def update_call(p, d):
    return pl.pallas_call(
        update_kernel,
        in_specs=[VMEM] * 2,
        out_specs=VMEM,
        out_shape=shape((p.shape[0], d.shape[1]), f32),
        compiler_params=params(8),
        name="update",
    )(p, d)


def final_kernel(places, inner, columns, entries, place, update, gate_weight, value_weight, *refs):
    count = len(places)
    shares, refs = refs[:columns], refs[columns:]
    weights, outs = refs[:count], refs[count : count + 6]
    gates, values, wide, narrow, sems, small_sems = refs[count + 6 :]
    new_gate, gate_step, gate_copy, new_value, value_step, value_copy = outs
    rows, split = gate_weight.shape
    both = shares[0][...]
    for share in shares[1:]:
        both = both + share[...]
    scale = [1.0 / (jnp.sqrt(both[i : i + 1, :1] / entries[i]) + rms_floor) for i in range(2)]
    z = lax.shift_right_logical(place[0], jnp.int32(inner.bit_length() - 1))
    x = lax.bitwise_and(place[0], jnp.int32(inner - 1))
    middle = is_middle(z)
    copies = []
    for i in range(count):
        (j, k), (middle_j, middle_k) = places[i]
        turn = jnp.int32(j) if j == middle_j else jnp.where(middle == 1, jnp.int32(middle_j), jnp.int32(j))
        flip = jnp.int32(k) if k == middle_k else jnp.where(middle == 1, jnp.int32(middle_k), jnp.int32(k))
        there = lax.bitwise_xor(z, turn) * inner + lax.bitwise_xor(x, flip)
        at = pl.ds(pl.multiple_of(there * rows, rows), rows)
        gate = update[at, :split] * scale[0]
        value = update[at, split:] * scale[1]
        old = weights[i][...].astype(f32)
        gates[i] = (old[:, :split] - learn_rate * gate).astype(bf16)
        values[i] = (old[:, split:] - learn_rate * value).astype(bf16)
        moves = [(gates.at[i], gate_copy.at[at], sems.at[i, 0]), (values.at[i], value_copy.at[at], sems.at[i, 1])]
        if i == 0:
            wide[0] = gate
            wide[1] = gate_weight[...] - learn_rate * gate
            narrow[0] = value
            narrow[1] = value_weight[...] - learn_rate * value
            outs = (wide, 0, gate_step), (wide, 1, new_gate), (narrow, 0, value_step), (narrow, 1, new_value)
            moves += [(held.at[n], out, small_sems.at[m]) for m, (held, n, out) in enumerate(outs)]
        for source, target, sem in moves:
            copies.append(pltpu.make_async_copy(source, target, sem))
            copies[-1].start()
    for copy in copies:
        copy.wait()


def final_call(place, places, weights, shares, update, gate_weight, value_weight, inner, columns):
    count = len(weights)
    rows, split = gate_weight.shape
    rest = value_weight.shape[1]
    depth = update.shape[0]
    entries = (depth * split * columns, depth * rest * columns)
    return pl.pallas_call(
        lambda *refs: final_kernel(places, inner, columns, entries, *refs),
        in_specs=[SMEM] + [VMEM] * (3 + len(shares) + count),
        out_specs=[HBM] * 6,
        out_shape=[
            shape((rows, split), f32),
            shape((rows, split), f32),
            shape((depth, split), bf16),
            shape((rows, rest), f32),
            shape((rows, rest), f32),
            shape((depth, rest), bf16),
        ],
        scratch_shapes=[
            pltpu.VMEM((count, rows, split), bf16),
            pltpu.VMEM((count, rows, rest), bf16),
            pltpu.VMEM((2, rows, split), f32),
            pltpu.VMEM((2, rows, rest), f32),
            pltpu.SemaphoreType.DMA((count, 2)),
            pltpu.SemaphoreType.DMA((4,)),
        ],
        compiler_params=params(12),
        name="final",
    )(place, update, gate_weight, value_weight, *shares, *weights)


def is_middle(z):
    return lax.bitwise_and(lax.bitwise_xor(z, lax.shift_right_logical(z, jnp.int32(1))), jnp.int32(1))


def pick_kernel(inner, place, first, second, out):
    middle = is_middle(lax.shift_right_logical(place[0], jnp.int32(inner.bit_length() - 1)))

    @pl.when(middle == 1)
    def _():
        out[...] = first[...]

    @pl.when(middle == 0)
    def _():
        out[...] = second[...]


def pick_call(place, first, second, inner):
    return pl.pallas_call(
        lambda *refs: pick_kernel(inner, *refs),
        in_specs=[SMEM] + [VMEM] * 2,
        out_specs=VMEM,
        out_shape=shape(first.shape, first.dtype),
        compiler_params=params(4),
    )(place, first, second)


def solution(mesh):
    fs, tp = mesh.shape["fs"], mesh.shape["tp"]
    inner = inner_of(fs)
    outer = fs // inner

    def gather(weight, place):
        if outer == 4 and inner == 2:
            across = lambda value: exchange(value, "fs", fs, 1)
            near = exchange(weight, "fs", fs, inner)
            side = lax.ppermute(weight, "fs", [(0, 1), (1, 0), (2, 4), (4, 2), (3, 5), (5, 3), (6, 7), (7, 6)])
            passed = exchange(side, "fs", fs, inner)
            far = lax.ppermute(near, "fs", [(0, 0), (1, 1), (2, 4), (4, 2), (3, 5), (5, 3), (6, 6), (7, 7)])
            last = pick_call(place, far, exchange(far, "fs", fs, inner), inner)
            weights = [
                weight,
                near,
                side,
                passed,
                across(pick_call(place, weight, near, inner)),
                across(pick_call(place, side, passed, inner)),
                last,
                across(last),
            ]
            distant = (0, 0), (1, 0), (0, 1), (2, 0), (1, 1), (2, 1), (3, 0), (3, 1)
            middle = (0, 0), (1, 0), (3, 0), (1, 1), (0, 1), (3, 1), (2, 0), (2, 1)
            return weights, tuple(zip(distant, middle))
        weights, places = [], []
        for j in range(outer):
            block = exchange(weight, "fs", fs, j * inner) if j else weight
            for k in range(inner):
                weights.append(exchange(block, "fs", fs, k) if k else block)
                places.append(((j, k), (j, k)))
        return weights, tuple(places)

    def per_device(
        normed_input,
        gate_cotangent,
        first_value_cot,
        second_value_cot,
        head_lambda,
        projection,
        gate_weight,
        gate_first,
        gate_second,
        value_weight,
        value_first,
        value_second,
    ):
        here = lax.axis_index("fs").astype(jnp.int32).reshape(1)
        weights, places = gather(cast_call(gate_weight, value_weight), here)
        halves = partial_call(
            here, normed_input, gate_cotangent, first_value_cot, second_value_cot, head_lambda, projection, outer, inner
        )
        upper, lower, half = gram_call(projection, halves[0])
        halves = [half] + [exchange(halves[k], "fs", fs, k) for k in range(1, inner)]
        parts = sum_call(halves)
        parts = [parts[0]] + [exchange(parts[j], "fs", fs, j * inner) for j in range(1, outer)]
        moments = gate_first, gate_second, value_first, value_second
        direction, low = direct_call(parts, moments)
        ngf, ngs, nvf, nvs = store_call(low, moments)
        slabs = {(0, 0): direction}
        for j in range(1, outer):
            slabs[j, 0] = exchange(direction, "fs", fs, j * inner)
        for j in range(outer):
            for k in range(1, inner):
                slabs[j, k] = exchange(slabs[j, 0], "fs", fs, k)
        full, squares = square_call(here, [slabs[j, k] for j in range(outer) for k in range(inner)], upper, lower, gate_cotangent.shape[1])
        shares = [squares] + [exchange(squares, "tp", tp, i) for i in range(1, tp)]
        new_gate, gate_step, gate_copy, new_value, value_step, value_copy = final_call(
            here,
            places,
            weights,
            shares,
            update_call(projection, full),
            gate_weight,
            value_weight,
            inner,
            tp,
        )
        return (
            new_gate,
            gate_step,
            gate_copy,
            ngf,
            ngs,
            new_value,
            value_step,
            value_copy,
            nvf,
            nvs,
        )

    blocked = P("fs", "tp")
    return jax.shard_map(
        per_device,
        mesh=mesh,
        in_specs=(P("fs", None), blocked, blocked, blocked, P("tp"), P()) + (blocked,) * 6,
        out_specs=(blocked, blocked, P(None, "tp"), blocked, blocked, blocked, blocked, P(None, "tp"), blocked, blocked),
        check_vma=False,
    )
```
